32 devices in a mesh: dp: 4 (over y, x), kv: 4 (over z), tp: 2 (over core).
Axes of the slice: x: 2, y: 2, z: 4, core: 2. Of those that a mesh axis runs over, the one named last changes fastest.
Arguments:
- tokens: bfloat16 [4, 1536, 2048], P('dp', 'kv'), may hold values from -21 to 21
- seq_lengths: int32 [4], P('dp'), may hold values from 1 to 1536, 2304 in all
- block_picks: int32 [4, 24, 4, 16], P('dp', 'kv', 'tp'), may hold values from -1 to 17, as said below
- w_query: bfloat16 [2048, 1024], P('kv', 'tp'), may hold values from -0.125 to 0.125
- w_key: bfloat16 [2048, 256], P('kv', 'tp'), may hold values from -0.125 to 0.125
- w_value: bfloat16 [2048, 256], P('kv', 'tp'), may hold values from -0.125 to 0.125
- w_gate: bfloat16 [2048, 32], replicated, may hold values from -0.125 to 0.125
- w_ckey: bfloat16 [4096, 64], replicated, may hold values from -0.09375 to 0.09375
- w_cvalue: bfloat16 [4096, 64], replicated, may hold values from -0.09375 to 0.09375
- w_out: bfloat16 [1024, 2048], P('tp', 'kv'), may hold values from -0.1875 to 0.1875
Outputs:
- attention_out: bfloat16 [4, 1536, 2048], P('dp', ('kv', 'tp'))
The draws below stay inside these ranges and needn't reach their ends.
Inputs may be any that keep to these rules, and one draw needn't show every extreme that they name: `block_picks`: A query block's entries name distinct blocks that all lie in earlier spans of 384 positions, or are -1; the largest such block is named in every draw. For one span and one group, the entries of all its query blocks together name blocks of any one other span at most 2 times; this is reached in every draw.
All inputs are finite; a program needn't handle non-finite values. No bound on the sum of `seq_lengths` on one device may be relied on, other than what follows from the above.
Results may differ from the reference program's by a relative error of at most 0.01.
The reference program's roundings to bfloat16 on the way count: a program that leaves them out, or rounds other values in their place, can miss the bound.
Values may be sent and summed in bfloat16 or wider, within the bound.
A program may use at most 64 MiB of HBM per device.

```python
import math
import jax
import jax.numpy as jnp
import numpy as np
from jax import lax

D = 2048
HEADS = 16
GROUPS = 4
HEAD = 64
BLK = 64
PICKS = 16
CAP = 2
TOK_DEV = 384
SEQS = 4
SEQ_LEN = 1536
HEAD_SETS = 2


def draw_tokens(key, part):
    grid_shape = (SEQS, SEQ_LEN, D)
    return jnp.clip(jax.random.normal(jax.random.fold_in(key, 20), grid_shape, jnp.float32), -6.0, 6.0).astype(jnp.bfloat16)


def draw_block_picks(key, part):
    span_count = SEQ_LEN // TOK_DEV
    per_span = TOK_DEV // BLK
    slot_total = per_span * PICKS
    grid_shape = (SEQS, span_count, GROUPS, span_count)
    random_order = jax.random.randint(jax.random.fold_in(key, 11), grid_shape, 0, 1 << 20)
    shifts = jax.random.randint(jax.random.fold_in(key, 12), grid_shape, 0, per_span)
    current = jnp.arange(span_count, dtype=jnp.int32)[None, :, None, None]
    candidate = jnp.arange(span_count, dtype=jnp.int32)[None, None, None, :]
    at_end = (current == span_count - 1) & (candidate == span_count - 2)
    shifts = jnp.where(at_end, per_span - 1, shifts)
    ranking = random_order * span_count + candidate
    ranking = jnp.where(candidate == 0, -3, ranking)
    ranking = jnp.where(candidate == current - 1, -4, ranking)
    ranking = jnp.where(candidate == current - span_count // 2, -1, ranking)
    ranking = jnp.where(candidate >= current, (1 << 20) * span_count + candidate, ranking)
    ordered = jnp.argsort(ranking, axis=-1).astype(jnp.int32)
    slots = jnp.arange(slot_total, dtype=jnp.int32)
    places = jnp.minimum(slots // CAP, span_count - 1)
    owners = jnp.take(ordered, places, axis=-1)
    offsets = jnp.take_along_axis(shifts, owners, axis=-1)
    inside = (offsets + slots % CAP) % per_span
    blocks = owners * per_span + inside
    is_valid = (slots // CAP)[None, None, None, :] < current
    picked = jnp.where(is_valid, blocks, -1)
    picked = picked.reshape(SEQS, span_count, GROUPS, per_span, PICKS).transpose(0, 1, 3, 2, 4)
    return picked.reshape(SEQS, span_count * per_span, GROUPS, PICKS).astype(jnp.int32)


def block_levels(own_key, shape, cuts, smallest, largest):
    gain = 1.0
    for dim, blocks in cuts:
        heights = jax.random.uniform(jax.random.fold_in(jax.random.fold_in(own_key, 6), dim), (blocks,), jnp.float32, smallest / len(cuts), largest / len(cuts))
        gain = gain * jnp.repeat(jnp.exp(heights), shape[dim] // blocks).reshape((-1,) + (1,) * (len(shape) - 1 - dim))
    return gain


def profile(number_of, total, limit, lean):
    portions = [(1 << 20) // math.isqrt(rank ** lean) + 1 for rank in range(2, number_of + 1)]
    rest, given = total - limit - (number_of - 1), [1] * (number_of - 1)
    while rest > 0:
        free = [i for i in range(number_of - 1) if given[i] < limit]
        whole, remaining = sum([portions[i] for i in free]), rest
        for i in free:
            extra = min(limit - given[i], max(1, remaining * portions[i] // whole), rest)
            given[i] = given[i] + extra
            rest = rest - extra
    return np.array([limit] + given)


def ragged(key, amount, total, reach, skew):
    if amount == 2:
        one = jax.random.randint(key, (), max(1, total - reach), min(reach, total - 1) + 1)
        return jnp.stack([one, total - one])
    tallies = jnp.asarray(profile(amount, total, reach, skew), jnp.int32)
    pairs = (amount - 1) // 2
    giver, receiver = tallies[1:1 + 2 * pairs:2], tallies[2:2 + 2 * pairs:2]
    room = jnp.minimum(giver - 1, reach - receiver)
    shifted = jax.random.randint(jax.random.fold_in(key, 1), (pairs,), 0, 1 << 20) % (room + 1)
    tallies = tallies.at[1:1 + 2 * pairs:2].set(giver - shifted).at[2:2 + 2 * pairs:2].set(receiver + shifted)
    return tallies[jax.random.permutation(jax.random.fold_in(key, 2), amount)]


def normal_values(stream_key, dims, scale, most, shards=(), held_as=jnp.bfloat16):
    drawn = scale * jax.random.normal(stream_key, dims, jnp.float32)
    if shards:
        drawn = drawn * block_levels(stream_key, dims, shards, -0.22, 0.18)
    return jnp.clip(drawn, -most, most).astype(held_as)


def setup_inputs(seed: int = 0) -> dict:
    key_of = jax.random.split(jax.random.key(seed), 11)
    tokens = draw_tokens(jax.random.fold_in(key_of[10], 71), 0)
    seq_lengths = ragged(key_of[1], SEQS, 3 * SEQS * SEQ_LEN // 8, SEQ_LEN, 2).astype(jnp.int32)
    block_picks = draw_block_picks(jax.random.fold_in(key_of[10], 71), 0)
    w_query = normal_values(key_of[3], (D, HEADS * HEAD), D ** -0.5, 0.125, ((0, 4), (1, 2)))
    w_key = normal_values(key_of[4], (D, GROUPS * HEAD), D ** -0.5, 0.125, ((0, 4), (1, 2)))
    w_value = normal_values(key_of[5], (D, GROUPS * HEAD), D ** -0.5, 0.125, ((0, 4), (1, 2)))
    w_gate = normal_values(key_of[6], (D, 2 * HEADS), D ** -0.5, 0.125)
    w_ckey = normal_values(key_of[7], (BLK * HEAD, HEAD), (BLK * HEAD) ** -0.5, 0.09375)
    w_cvalue = normal_values(key_of[8], (BLK * HEAD, HEAD), (BLK * HEAD) ** -0.5, 0.09375)
    w_out = normal_values(key_of[9], (HEADS * HEAD, D), (HEADS * HEAD) ** -0.5, 0.1875, ((0, 2), (1, 4)))
    return dict(tokens=tokens, seq_lengths=seq_lengths, block_picks=block_picks, w_query=w_query, w_key=w_key, w_value=w_value, w_gate=w_gate, w_ckey=w_ckey, w_cvalue=w_cvalue, w_out=w_out)


masked_low = -1e30


def reference(tokens, seq_lengths, block_picks, w_query, w_key, w_value, w_gate, w_ckey, w_cvalue, w_out):
    per_group = HEADS // GROUPS
    block_total = SEQ_LEN // BLK
    inv_scale = HEAD ** -0.5
    set_width = HEADS * HEAD // HEAD_SETS
    causal = jnp.arange(BLK)[None, :] <= jnp.arange(BLK)[:, None]
    block_ends = jnp.arange(block_total, dtype=jnp.int32) * BLK + (BLK - 1)
    group_ids = jnp.arange(GROUPS, dtype=jnp.int32)

    def sequence(inputs):
        token_rows, length, picked = inputs
        queries = jnp.dot(token_rows, w_query, preferred_element_type=jnp.float32).astype(jnp.bfloat16)
        queries = lax.optimization_barrier(queries).reshape(block_total, BLK, GROUPS, per_group, HEAD)
        keys_all = jnp.dot(token_rows, w_key, preferred_element_type=jnp.float32).astype(jnp.bfloat16)
        keys_all = keys_all.reshape(block_total, BLK, GROUPS, HEAD).transpose(0, 2, 1, 3)
        values_all = jnp.dot(token_rows, w_value, preferred_element_type=jnp.float32).astype(jnp.bfloat16)
        values_all = values_all.reshape(block_total, BLK, GROUPS, HEAD).transpose(0, 2, 1, 3)
        keys_all = lax.optimization_barrier(keys_all)
        values_all = lax.optimization_barrier(values_all)
        gate_all = jax.nn.sigmoid(jnp.dot(token_rows, w_gate, preferred_element_type=jnp.float32))
        gate_all = gate_all.reshape(block_total, BLK, 2, GROUPS, per_group)
        ckeys = jnp.dot(keys_all.reshape(block_total * GROUPS, BLK * HEAD), w_ckey,
                        preferred_element_type=jnp.float32).astype(jnp.bfloat16)
        cvalues = jnp.dot(values_all.reshape(block_total * GROUPS, BLK * HEAD), w_cvalue,
                          preferred_element_type=jnp.float32).astype(jnp.bfloat16)
        ckeys = lax.optimization_barrier(ckeys).reshape(block_total, GROUPS, HEAD).astype(jnp.float32)
        cvalues = lax.optimization_barrier(cvalues).reshape(block_total, GROUPS, HEAD).astype(jnp.float32)

        def attend(block_inputs):
            qblock, gblock, picked_row, block_index = block_inputs
            qfloat = qblock.astype(jnp.float32)
            query_spots = block_index * BLK + jnp.arange(BLK, dtype=jnp.int32)
            comp_score = jnp.einsum('tgpd,cgd->gtpc', qfloat, ckeys) * inv_scale
            visible = (block_ends[None, :] <= query_spots[:, None])[None, :, None, :]
            comp_score = jnp.where(visible, comp_score, masked_low)
            comp_top = jnp.max(comp_score, axis=-1, keepdims=True)
            comp_weight = jnp.where(visible, jnp.exp(comp_score - comp_top), 0.0)
            comp_sum = jnp.maximum(jnp.sum(comp_weight, axis=-1, keepdims=True), 1.0)
            comp_prob = lax.optimization_barrier((comp_weight / comp_sum).astype(jnp.bfloat16))
            comp_out = jnp.einsum('gtpc,cgd->tgpd', comp_prob.astype(jnp.float32), cvalues)
            own_keys = keys_all[block_index].astype(jnp.float32)
            own_values = values_all[block_index].astype(jnp.float32)
            usable = picked_row >= 0
            safe_picks = jnp.where(usable, picked_row, 0)
            far_keys = keys_all[safe_picks, group_ids[:, None]].reshape(GROUPS, PICKS * BLK, HEAD).astype(jnp.float32)
            far_values = values_all[safe_picks, group_ids[:, None]].reshape(GROUPS, PICKS * BLK, HEAD).astype(jnp.float32)
            own_score = jnp.einsum('tgpd,gsd->gtps', qfloat, own_keys) * inv_scale
            own_mask = causal[None, :, None, :]
            own_score = jnp.where(own_mask, own_score, masked_low)
            far_score = jnp.einsum('tgpd,gkd->gtpk', qfloat, far_keys) * inv_scale
            far_mask = jnp.repeat(usable, BLK, axis=-1)[:, None, None, :]
            far_score = jnp.where(far_mask, far_score, masked_low)
            score_top = jnp.maximum(jnp.max(own_score, axis=-1, keepdims=True),
                                    jnp.max(far_score, axis=-1, keepdims=True))
            own_weight = jnp.where(own_mask, jnp.exp(own_score - score_top), 0.0)
            far_weight = jnp.where(far_mask, jnp.exp(far_score - score_top), 0.0)
            normalizer = jnp.sum(own_weight, axis=-1, keepdims=True) + jnp.sum(far_weight, axis=-1, keepdims=True)
            own_prob = lax.optimization_barrier((own_weight / normalizer).astype(jnp.bfloat16))
            far_prob = lax.optimization_barrier((far_weight / normalizer).astype(jnp.bfloat16))
            chosen_out = (jnp.einsum('gtps,gsd->tgpd', own_prob.astype(jnp.float32), own_values)
                          + jnp.einsum('gtpk,gkd->tgpd', far_prob.astype(jnp.float32), far_values))
            mixed_out = gblock[:, 0, :, :, None] * comp_out + gblock[:, 1, :, :, None] * chosen_out
            return mixed_out.astype(jnp.bfloat16)

        attended = lax.map(attend, (queries, gate_all, picked, jnp.arange(block_total, dtype=jnp.int32)))
        attended = attended.reshape(SEQ_LEN, HEAD_SETS, set_width)
        weight_sets = w_out.reshape(HEAD_SETS, set_width, D)
        summed = jnp.zeros((SEQ_LEN, D), jnp.float32)
        for set_index in range(HEAD_SETS):
            partial_out = jnp.dot(attended[:, set_index], weight_sets[set_index],
                                  preferred_element_type=jnp.float32).astype(jnp.bfloat16)
            summed = summed + lax.optimization_barrier(partial_out).astype(jnp.float32)
        live_rows = jnp.arange(SEQ_LEN, dtype=jnp.int32) < length
        return jnp.where(live_rows[:, None], summed, 0.0).astype(jnp.bfloat16)

    return lax.map(sequence, (tokens, seq_lengths, block_picks))
```

```python
import functools

import jax
import jax.numpy as jnp
from jax import lax
from jax.experimental import pallas as pl
from jax.experimental.pallas import tpu as pltpu
from jax.sharding import PartitionSpec as P

HEAD = 64
BLK = 64
CAP = 2
LANES = 128
PAD = 16
masked_low = -1e30
BF = jnp.bfloat16
F32 = jnp.float32


class Ring:
    def __init__(self, sizes, buf, rows, sems, share):
        self.n, self.buf, self.share = sizes["kv"], buf, share
        self.me = lax.axis_index("kv")
        self.dp = lax.axis_index("dp")
        n = self.n
        if share:
            self.piece = rows // 4
            self.parity = lax.rem(self.dp + self.dp // 2, 2)
            self.plans = []
            for way in (0, 1):
                plan = []
                for step in range(1, n // 2 + 1):
                    if 2 * step == n:
                        plan.append([way])
                    else:
                        plan.append([0, 1] if way == 0 else [1, 0])
                self.plans.append(plan)
        else:
            self.piece = rows
            self.parity = 0
            self.plans = [[[0] for _ in range(1, n)], []]
        self.zs, self.zr, self.fs, self.fr = sems
        self.started = []

    def rows_of(self, parity, i):
        if not self.share:
            return pl.ds(0, self.piece)
        return pl.ds(pl.multiple_of((2 * parity + i) * self.piece, self.piece), self.piece)

    def hop(self, way, step, i):
        n = self.n
        sign = 1 if way == 0 else -1
        owner = lax.rem(self.me - sign * (step - 1) + n, n)
        target = lax.rem(self.me + sign + n, n)
        at = self.buf.at[owner, self.rows_of(self.parity, i)]
        return pltpu.make_async_remote_copy(
            src_ref=at,
            dst_ref=at,
            send_sem=self.zs.at[way, step - 1, i],
            recv_sem=self.zr.at[way, step - 1, i],
            device_id={"kv": target},
            device_id_type=pl.DeviceIdType.MESH,
        )

    def arrival(self, way, step, i):
        n = self.n
        sign = 1 if way == 0 else -1
        owner = lax.rem(self.me - sign * step + n, n)
        at = self.buf.at[owner, self.rows_of(self.parity, i)]
        return pltpu.make_async_remote_copy(
            src_ref=at,
            dst_ref=at,
            send_sem=self.zs.at[way, step - 1, i],
            recv_sem=self.zr.at[way, step - 1, i],
            device_id={"kv": lax.rem(self.me + sign + n, n)},
            device_id_type=pl.DeviceIdType.MESH,
        )

    def pass_on(self, way, step, i, parity):
        n = self.n
        sign = 1 if way == 0 else -1
        owner = lax.rem(self.me - sign * step + n, n)
        at = self.buf.at[owner, self.rows_of(parity, i)]
        bit = 1 if i == 0 else 2
        low = lax.rem(self.dp, 2)
        high = self.dp // 2
        other = (high * 2 + 1 - low) if bit == 1 else ((1 - high) * 2 + low)
        return pltpu.make_async_remote_copy(
            src_ref=at,
            dst_ref=at,
            send_sem=self.fs.at[way, step - 1, i],
            recv_sem=self.fr.at[way, step - 1, i],
            device_id={"dp": other},
            device_id_type=pl.DeviceIdType.MESH,
        )

    def items(self):
        out = []
        deep = max(len(p) for p in self.plans)
        for step in range(1, deep + 1):
            for rank in range(2):
                for way in (0, 1):
                    plan = self.plans[way]
                    if step <= len(plan) and rank < len(plan[step - 1]):
                        out.append((way, step, plan[step - 1][rank]))
        return out

    def begin(self):
        for way, step, i in self.items():
            if step == 1:
                self.hop(way, 1, i).start()

    def relay(self):
        for way, step, i in self.items():
            self.arrival(way, step, i).wait_recv()
            plan = self.plans[way]
            if step < len(plan) and i in plan[step]:
                self.hop(way, step + 1, i).start()
            if self.share:
                self.pass_on(way, step, i, self.parity).start()

    def finish(self):
        if self.share:
            for way, step, i in self.items():
                self.pass_on(way, step, i, 1 - self.parity).wait_recv()

    def drain(self):
        for way, step, i in self.items():
            self.hop(way, step, i).wait_send()
            if self.share:
                self.pass_on(way, step, i, self.parity).wait_send()


def kernel(
    sizes,
    share,
    seq_ref,
    picks_ref,
    tokens_ref,
    wq_ref,
    wk_ref,
    wv_ref,
    wg_ref,
    wck_ref,
    wcv_ref,
    wo_ref,
    out_ref,
    tok,
    wall,
    wout,
    wgate,
    wck,
    wcv,
    queries,
    kv32,
    kv_all,
    flat,
    comp_all,
    gates,
    att,
    near,
    sendbuf,
    recvbuf,
    slots,
    local_sem,
    qs1,
    qr1,
    qs2,
    qr2,
    os1,
    or1,
    os2,
    or2,
    ks,
    kr,
    cs,
    cr,
    ts,
    tr,
):
    n = sizes["kv"]
    me = lax.axis_index("kv")
    tp = lax.axis_index("tp")
    dp = lax.axis_index("dp")
    count = tok.shape[0]
    blocks = count // BLK
    width = tok.shape[1]
    qcols = wq_ref.shape[1]
    heads = qcols // HEAD
    groups = wk_ref.shape[1] // HEAD
    per_group = heads // groups
    all_heads = wg_ref.shape[1] // 2
    picks = picks_ref.shape[3]
    depth = slots.shape[2]
    half = count // 2
    MESH = pl.DeviceIdType.MESH

    locals_ = [
        pltpu.make_async_copy(wq_ref, wall.at[me, :, pl.ds(0, qcols)], local_sem.at[0]),
        pltpu.make_async_copy(wk_ref, wall.at[me, :, pl.ds(qcols, LANES)], local_sem.at[1]),
        pltpu.make_async_copy(wv_ref, wall.at[me, :, pl.ds(qcols + LANES, LANES)], local_sem.at[2]),
        pltpu.make_async_copy(wo_ref, wout.at[me], local_sem.at[3]),
        pltpu.make_async_copy(tokens_ref.at[0], tok, local_sem.at[4]),
        pltpu.make_async_copy(wg_ref, wgate, local_sem.at[5]),
        pltpu.make_async_copy(wck_ref, wck, local_sem.at[6]),
        pltpu.make_async_copy(wcv_ref, wcv, local_sem.at[7]),
    ]
    for copy in locals_:
        copy.start()

    barrier = pltpu.get_barrier_semaphore()
    greeted = 0
    for d in range(1, n):
        pl.semaphore_signal(barrier, inc=1, device_id={"kv": lax.rem(me + d, n)}, device_id_type=MESH)
        greeted += 1
    pl.semaphore_signal(barrier, inc=1, device_id={"tp": 1 - tp}, device_id_type=MESH)
    greeted += 1
    if share:
        low, high = lax.rem(dp, 2), dp // 2
        for other in (high * 2 + 1 - low, (1 - high) * 2 + low):
            pl.semaphore_signal(barrier, inc=1, device_id={"dp": other}, device_id_type=MESH)
            greeted += 1
    pl.semaphore_wait(barrier, greeted)

    ring = Ring(sizes, wall, wall.shape[1], (qs1, qr1, qs2, qr2), share)
    oring = Ring(sizes, wout, wout.shape[1], (os1, or1, os2, or2), share)
    for copy in locals_[:3]:
        copy.wait()
    ring.begin()

    @pl.loop(0, blocks)
    def _(b):
        for g in range(groups):
            entries = [picks_ref[0, b, g, k] for k in range(picks)]
            last = jnp.int32(2**30)
            for s in range(depth):
                best = jnp.int32(-1)
                for entry in entries:
                    best = jnp.maximum(best, jnp.where(entry < last, entry, -1))
                slots[b, g, s] = best
                last = best

    for copy in locals_[3:]:
        copy.wait()
    gates[...] = jax.nn.sigmoid(jnp.dot(tok[...], wgate[...], preferred_element_type=F32))
    ring.relay()
    oring.begin()
    ring.finish()

    every = wall[...].reshape(width, wall.shape[2])
    kvsum = jnp.dot(tok[...], every[:, qcols:], preferred_element_type=F32).astype(BF)
    kv_all[pl.ds(me * blocks, blocks)] = kvsum.reshape(blocks, BLK, 2 * LANES)
    kv32[0] = kvsum[:, :LANES].astype(F32)
    kv32[1] = kvsum[:, LANES:].astype(F32)
    qsum = jnp.dot(tok[...], every[:, :qcols], preferred_element_type=F32)
    queries[...] = qsum.astype(BF).astype(F32)

    def kv_copy(d, slot):
        return pltpu.make_async_remote_copy(
            src_ref=kv_all.at[pl.ds(slot * blocks, blocks)],
            dst_ref=kv_all.at[pl.ds(slot * blocks, blocks)],
            send_sem=ks.at[d],
            recv_sem=kr.at[d],
            device_id={"kv": lax.rem(me + d, n)},
            device_id_type=MESH,
        )

    def comp_copy(d, slot):
        return pltpu.make_async_remote_copy(
            src_ref=comp_all.at[slot],
            dst_ref=comp_all.at[slot],
            send_sem=cs.at[d],
            recv_sem=cr.at[d],
            device_id={"kv": lax.rem(me + d, n)},
            device_id_type=MESH,
        )

    for d in range(1, n):

        @pl.when(me + d < n)
        def _():
            kv_copy(d, me).start()

    left = lax.broadcasted_iota(jnp.int32, (blocks, LANES), 1) < HEAD
    parts = []
    for which, weights in ((0, wck), (1, wcv)):
        source = kv32.at[which]
        flat[...] = jnp.zeros_like(flat)
        for pair in range(BLK // 2):
            even = source[pl.ds(2 * pair, blocks, stride=BLK), :]
            odd = source[pl.ds(2 * pair + 1, blocks, stride=BLK), :]
            span = pl.ds(pair * LANES, LANES)
            flat[0, 0:blocks, span] = jnp.where(left, even, pltpu.roll(odd, HEAD, 1))
            flat[1, 0:blocks, span] = jnp.where(left, pltpu.roll(even, HEAD, 1), odd)
        for g in range(groups):
            parts.append(jnp.dot(flat[g].astype(BF), weights[...], preferred_element_type=F32))
    comp_all[me] = jnp.concatenate(parts, axis=1).astype(BF)
    for d in range(1, n):
        comp_copy(d, me).start()

    oring.relay()

    for d in range(1, n):

        @pl.when(me - d >= 0)
        def _():
            kv_copy(d, lax.rem(me - d + n, n)).wait_recv()

        comp_copy(d, lax.rem(me - d + n, n)).wait_recv()

    rows = per_group * BLK
    comp_pairs = comp_all[...].reshape(n * PAD, 2 * LANES)
    nkeys = (1 + depth) * BLK
    lane64 = lax.broadcasted_iota(jnp.int32, (BLK, LANES), 1) < HEAD
    dims = (((1,), (1,)), ((), ()))
    comp_lane = lax.broadcasted_iota(jnp.int32, (rows, n * PAD), 1)
    comp_spot = lax.rem(lax.broadcasted_iota(jnp.int32, (rows, n * PAD), 0), BLK)
    comp_block = (comp_lane // PAD) * blocks + lax.rem(comp_lane, PAD)
    comp_real = lax.rem(comp_lane, PAD) < blocks
    key_lane = lax.broadcasted_iota(jnp.int32, (1, nkeys), 1)
    own_lane = lax.broadcasted_iota(jnp.int32, (rows, nkeys), 1)
    own_spot = lax.rem(lax.broadcasted_iota(jnp.int32, (rows, nkeys), 0), BLK)
    hidden = jnp.logical_and(own_lane < BLK, own_lane > own_spot)

    for b in range(blocks):
        spot = pl.ds(b * BLK, BLK)
        for g in range(groups):
            stacked = []
            for i in range(per_group):
                h = g * per_group + i
                tile = queries[spot, pl.ds((h // 2) * LANES, LANES)] * (HEAD**-0.5)
                if h % 2 != g:
                    tile = pltpu.roll(tile, HEAD, 1)
                keep = lane64 if g == 0 else jnp.logical_not(lane64)
                stacked.append(jnp.where(keep, tile, 0.0))
            qrows = jnp.concatenate(stacked, axis=0).astype(BF)

            comp_score = lax.dot_general(qrows, comp_pairs[:, :LANES], dims, preferred_element_type=F32)
            visible = jnp.logical_and(
                comp_real, (comp_block + 1) * BLK - 1 <= me * count + b * BLK + comp_spot
            )
            comp_score = jnp.where(visible, comp_score, masked_low)
            comp_top = jnp.max(comp_score, axis=1, keepdims=True)
            comp_weight = jnp.where(visible, jnp.exp(comp_score - comp_top), 0.0)
            comp_sum = jnp.maximum(jnp.sum(comp_weight, axis=1, keepdims=True), 1.0)
            comp_prob = (comp_weight / comp_sum).astype(BF)
            comp_out = jnp.dot(comp_prob, comp_pairs[:, LANES:], preferred_element_type=F32)

            near[0:BLK, :] = kv_all[me * blocks + b]
            bias = jnp.zeros((1, nkeys), F32)
            named = [slots[b, g, s] for s in range(depth)]

            def pickup(c, held):
                block = kv_all[c]
                return tuple(lax.select(pick == c, block, old) for pick, old in zip(named, held))

            nothing = jnp.zeros((BLK, 2 * LANES), BF)
            found = lax.fori_loop(0, me * blocks, pickup, (nothing,) * depth)
            for s in range(depth):
                near[(s + 1) * BLK : (s + 2) * BLK, :] = found[s]
                shut = jnp.where(named[s] < 0, masked_low, 0.0)
                bias = jnp.where(key_lane // BLK == s + 1, shut, bias)
            score = lax.dot_general(qrows, near[:, :LANES], dims, preferred_element_type=F32) + bias
            score = jnp.where(hidden, masked_low, score)
            top = jnp.max(score, axis=1, keepdims=True)
            weight = jnp.exp(score - top)
            prob = (weight / jnp.sum(weight, axis=1, keepdims=True)).astype(BF)
            chosen_out = jnp.dot(prob, near[:, LANES:], preferred_element_type=F32)

            cols = [[], []]
            for i in range(per_group):
                for branch in (0, 1):
                    first = branch * all_heads + g * per_group + i
                    a = gates[spot, first : first + 1]
                    c = gates[spot, first + heads : first + heads + 1]
                    cols[branch].append(jnp.where(tp == 0, a, c))
            mixed = (
                jnp.concatenate(cols[0], axis=0) * comp_out
                + jnp.concatenate(cols[1], axis=0) * chosen_out
            )
            for j in range(per_group // 2):
                even = mixed[2 * j * BLK : (2 * j + 1) * BLK]
                odd = mixed[(2 * j + 1) * BLK : (2 * j + 2) * BLK]
                if g == 0:
                    odd = pltpu.roll(odd, HEAD, 1)
                else:
                    even = pltpu.roll(even, HEAD, 1)
                tile = g * (per_group // 2) + j
                att[spot, tile * LANES : (tile + 1) * LANES] = jnp.where(lane64, even, odd).astype(BF)

    oring.finish()

    def back(o):
        return pltpu.make_async_remote_copy(
            src_ref=sendbuf.at[o],
            dst_ref=recvbuf.at[o],
            send_sem=ts.at[o],
            recv_sem=tr.at[o],
            device_id={"tp": 1 - tp},
            device_id_type=MESH,
        )

    theirs = att[pl.ds(pl.multiple_of((1 - tp) * half, half), half), :]
    mine = att[pl.ds(pl.multiple_of(tp * half, half), half), :]
    for o in range(n):
        sendbuf[o] = jnp.dot(theirs, wout[o], preferred_element_type=F32).astype(BF)
        back(o).start()
    cols_each = wout.shape[2]
    live = (
        me * count + tp * half + lax.broadcasted_iota(jnp.int32, (half, cols_each), 0)
    ) < seq_ref[0]
    for o in range(n):
        kept = jnp.dot(mine, wout[o], preferred_element_type=F32).astype(BF).astype(F32)
        back(o).wait_recv()
        total = kept + recvbuf[o].astype(F32)
        out_ref[0, :, o * cols_each : (o + 1) * cols_each] = jnp.where(live, total, 0.0).astype(BF)

    ring.drain()
    oring.drain()
    for d in range(1, n):

        @pl.when(me + d < n)
        def _():
            kv_copy(d, me).wait_send()

        comp_copy(d, me).wait_send()
    for o in range(n):
        back(o).wait_send()


def solution(mesh):
    sizes = dict(mesh.shape)
    n = sizes["kv"]

    def body(tokens, seq_lengths, block_picks, wq, wk, wv, wg, wck, wcv, wo):
        _, count, width = tokens.shape
        blocks = count // BLK
        groups = wk.shape[1] // HEAD
        share = sizes["dp"] == 4 and (wq.shape[0] // 4) % 16 == 0 and n % 2 == 0
        steps = (2, n // 2, 2) if share else (1, n - 1, 1)
        depth = min(block_picks.shape[3], CAP * (n - 1))
        cols = wq.shape[1] + wk.shape[1] + wv.shape[1]
        half = count // sizes["tp"]
        sem = pltpu.SemaphoreType.DMA
        return pl.pallas_call(
            functools.partial(kernel, sizes, share),
            out_shape=jax.ShapeDtypeStruct((1, half, wo.shape[1] * n), BF),
            in_specs=[pl.BlockSpec(memory_space=pltpu.SMEM)] * 2
            + [pl.BlockSpec(memory_space=pl.ANY)] * 8,
            out_specs=pl.BlockSpec(memory_space=pltpu.VMEM),
            scratch_shapes=[
                pltpu.VMEM((count, width), BF),
                pltpu.VMEM((n, wq.shape[0], cols), BF),
                pltpu.VMEM((n,) + wo.shape, BF),
                pltpu.VMEM(wg.shape, BF),
                pltpu.VMEM(wck.shape, BF),
                pltpu.VMEM(wcv.shape, BF),
                pltpu.VMEM((count, wq.shape[1]), F32),
                pltpu.VMEM((2, count, LANES), F32),
                pltpu.VMEM((n * blocks, BLK, 2 * LANES), BF),
                pltpu.VMEM((groups, PAD, BLK * HEAD), F32),
                pltpu.VMEM((n, PAD, 2 * LANES), BF),
                pltpu.VMEM((count, wg.shape[1]), F32),
                pltpu.VMEM((count, wq.shape[1]), BF),
                pltpu.VMEM(((1 + depth) * BLK, 2 * LANES), BF),
                pltpu.VMEM((n, half, wo.shape[1]), BF),
                pltpu.VMEM((n, half, wo.shape[1]), BF),
                pltpu.SMEM((blocks, groups, depth), jnp.int32),
                sem((8,)),
            ]
            + [sem(steps)] * 8
            + [sem((n,))] * 6,
            compiler_params=pltpu.CompilerParams(
                collective_id=0, has_side_effects=True, vmem_limit_bytes=60 * 1024 * 1024
            ),
        )(seq_lengths, block_picks, tokens, wq, wk, wv, wg, wck, wcv, wo)

    return jax.shard_map(
        body,
        mesh=mesh,
        in_specs=(
            P("dp", "kv", None),
            P("dp"),
            P("dp", "kv", "tp", None),
            P("kv", "tp"),
            P("kv", "tp"),
            P("kv", "tp"),
            P(),
            P(),
            P(),
            P("tp", "kv"),
        ),
        out_specs=P("dp", ("kv", "tp"), None),
        check_vma=False,
    )
```

```python
import functools

import jax
import jax.numpy as jnp
from jax import lax
from jax.experimental import pallas as pl
from jax.experimental.pallas import tpu as pltpu
from jax.sharding import PartitionSpec as P

HEAD = 64
BLK = 64
CAP = 2
LANES = 128
PAD = 16
masked_low = -1e30
BF = jnp.bfloat16
F32 = jnp.float32


class Ring:
    def __init__(self, sizes, buf, rows, sems, share):
        self.n, self.buf, self.share = sizes["kv"], buf, share
        self.me = lax.axis_index("kv")
        self.dp = lax.axis_index("dp")
        n = self.n
        if share:
            self.piece = rows // 4
            self.parity = lax.rem(self.dp + self.dp // 2, 2)
            self.plans = []
            for way in (0, 1):
                plan = []
                for step in range(1, n // 2 + 1):
                    if 2 * step == n:
                        plan.append([way])
                    else:
                        plan.append([0, 1] if way == 0 else [1, 0])
                self.plans.append(plan)
        else:
            self.piece = rows
            self.parity = 0
            self.plans = [[[0] for _ in range(1, n)], []]
        self.zs, self.zr, self.fs, self.fr = sems
        self.started = []

    def rows_of(self, parity, i):
        if not self.share:
            return pl.ds(0, self.piece)
        return pl.ds(pl.multiple_of((2 * parity + i) * self.piece, self.piece), self.piece)

    def hop(self, way, step, i):
        n = self.n
        sign = 1 if way == 0 else -1
        owner = lax.rem(self.me - sign * (step - 1) + n, n)
        target = lax.rem(self.me + sign + n, n)
        at = self.buf.at[owner, self.rows_of(self.parity, i)]
        return pltpu.make_async_remote_copy(
            src_ref=at,
            dst_ref=at,
            send_sem=self.zs.at[way, step - 1, i],
            recv_sem=self.zr.at[way, step - 1, i],
            device_id={"kv": target},
            device_id_type=pl.DeviceIdType.MESH,
        )

    def arrival(self, way, step, i):
        n = self.n
        sign = 1 if way == 0 else -1
        owner = lax.rem(self.me - sign * step + n, n)
        at = self.buf.at[owner, self.rows_of(self.parity, i)]
        return pltpu.make_async_remote_copy(
            src_ref=at,
            dst_ref=at,
            send_sem=self.zs.at[way, step - 1, i],
            recv_sem=self.zr.at[way, step - 1, i],
            device_id={"kv": lax.rem(self.me + sign + n, n)},
            device_id_type=pl.DeviceIdType.MESH,
        )

    def pass_on(self, way, step, i, parity):
        n = self.n
        sign = 1 if way == 0 else -1
        owner = lax.rem(self.me - sign * step + n, n)
        at = self.buf.at[owner, self.rows_of(parity, i)]
        bit = 1 if i == 0 else 2
        low = lax.rem(self.dp, 2)
        high = self.dp // 2
        other = (high * 2 + 1 - low) if bit == 1 else ((1 - high) * 2 + low)
        return pltpu.make_async_remote_copy(
            src_ref=at,
            dst_ref=at,
            send_sem=self.fs.at[way, step - 1, i],
            recv_sem=self.fr.at[way, step - 1, i],
            device_id={"dp": other},
            device_id_type=pl.DeviceIdType.MESH,
        )

    def items(self):
        out = []
        deep = max(len(p) for p in self.plans)
        for step in range(1, deep + 1):
            for rank in range(2):
                for way in (0, 1):
                    plan = self.plans[way]
                    if step <= len(plan) and rank < len(plan[step - 1]):
                        out.append((way, step, plan[step - 1][rank]))
        return out

    def begin(self):
        for way, step, i in self.items():
            if step == 1:
                self.hop(way, 1, i).start()

    def relay(self, first=0, last=None):
        for way, step, i in self.items()[first:last]:
            self.arrival(way, step, i).wait_recv()
            plan = self.plans[way]
            if step < len(plan) and i in plan[step]:
                self.hop(way, step + 1, i).start()
            if self.share:
                self.pass_on(way, step, i, self.parity).start()

    def finish(self):
        if self.share:
            for way, step, i in self.items():
                self.pass_on(way, step, i, 1 - self.parity).wait_recv()

    def drain(self):
        for way, step, i in self.items():
            self.hop(way, step, i).wait_send()
            if self.share:
                self.pass_on(way, step, i, self.parity).wait_send()


def kernel(
    sizes,
    share,
    seq_ref,
    picks_ref,
    tokens_ref,
    wq_ref,
    wk_ref,
    wv_ref,
    wg_ref,
    wck_ref,
    wcv_ref,
    wo_ref,
    out_ref,
    tok,
    wall,
    wout,
    wgate,
    wck,
    wcv,
    queries,
    kv32,
    kv_all,
    flat,
    comp_all,
    gates,
    att,
    near,
    sendbuf,
    recvbuf,
    slots,
    shuts,
    local_sem,
    qs1,
    qr1,
    qs2,
    qr2,
    os1,
    or1,
    os2,
    or2,
    ks,
    kr,
    cs,
    cr,
    ts,
    tr,
):
    n = sizes["kv"]
    me = lax.axis_index("kv")
    tp = lax.axis_index("tp")
    dp = lax.axis_index("dp")
    count = tok.shape[0]
    blocks = count // BLK
    width = tok.shape[1]
    qcols = wq_ref.shape[1]
    heads = qcols // HEAD
    groups = wk_ref.shape[1] // HEAD
    per_group = heads // groups
    all_heads = wg_ref.shape[0] // 2
    picks = picks_ref.shape[3]
    depth = slots.shape[2]
    half = count // 2
    MESH = pl.DeviceIdType.MESH
    dims = (((1,), (1,)), ((), ()))

    locals_ = [
        pltpu.make_async_copy(wq_ref, wall.at[me, :, pl.ds(0, qcols)], local_sem.at[0]),
        pltpu.make_async_copy(wk_ref, wall.at[me, :, pl.ds(qcols, LANES)], local_sem.at[1]),
        pltpu.make_async_copy(wv_ref, wall.at[me, :, pl.ds(qcols + LANES, LANES)], local_sem.at[2]),
        pltpu.make_async_copy(wo_ref, wout.at[me], local_sem.at[3]),
        pltpu.make_async_copy(tokens_ref.at[0], tok, local_sem.at[4]),
        pltpu.make_async_copy(wg_ref, wgate, local_sem.at[5]),
        pltpu.make_async_copy(wck_ref, wck, local_sem.at[6]),
        pltpu.make_async_copy(wcv_ref, wcv, local_sem.at[7]),
    ]
    for copy in locals_:
        copy.start()

    barrier = pltpu.get_barrier_semaphore()
    greeted = 0
    for d in range(1, n):
        pl.semaphore_signal(barrier, inc=1, device_id={"kv": lax.rem(me + d, n)}, device_id_type=MESH)
        greeted += 1
    pl.semaphore_signal(barrier, inc=1, device_id={"tp": 1 - tp}, device_id_type=MESH)
    greeted += 1
    if share:
        low, high = lax.rem(dp, 2), dp // 2
        for other in (high * 2 + 1 - low, (1 - high) * 2 + low):
            pl.semaphore_signal(barrier, inc=1, device_id={"dp": other}, device_id_type=MESH)
            greeted += 1
    pl.semaphore_wait(barrier, greeted)

    ring = Ring(sizes, wall, wall.shape[1], (qs1, qr1, qs2, qr2), share)
    oring = Ring(sizes, wout, wout.shape[1], (os1, or1, os2, or2), share)
    for copy in locals_[:3]:
        copy.wait()
    ring.begin()

    together = CAP * (n - 1) <= picks
    for g in range(groups if together else 0):
        last = jnp.int32(2**30)
        for s in range(depth):

            def scan(b, best):
                for k in range(picks):
                    entry = picks_ref[0, b, g, k]
                    best = jnp.maximum(best, jnp.where(entry < last, entry, -1))
                return best

            last = lax.fori_loop(0, blocks, scan, jnp.int32(-1))
            slots[0, g, s] = last

    @pl.loop(0, blocks)
    def _(b):
        for g in range(groups):
            entries = [picks_ref[0, b, g, k] for k in range(picks)]
            last = jnp.int32(2**30)
            for s in range(depth):
                if together:
                    best = slots[0, g, s]
                    hits = jnp.int32(0)
                    for entry in entries:
                        hits = jnp.maximum(hits, jnp.where(entry == best, 1, 0))
                    hits = jnp.where(best < 0, 0, hits)
                    shuts[b, g, s] = jnp.where(hits > 0, 0.0, masked_low)
                else:
                    best = jnp.int32(-1)
                    for entry in entries:
                        best = jnp.maximum(best, jnp.where(entry < last, entry, -1))
                    slots[b, g, s] = best
                    shuts[b, g, s] = jnp.where(best < 0, masked_low, 0.0)
                    last = best

    for copy in locals_[3:]:
        copy.wait()
    gates[...] = jax.nn.sigmoid(
        lax.dot_general(tok[...], wgate[...], dims, preferred_element_type=F32)
    )
    ring.relay()
    oring.begin()
    ring.finish()

    every = wall[...].reshape(width, wall.shape[2])
    kvsum = jnp.dot(tok[...], every[:, qcols:], preferred_element_type=F32).astype(BF)
    kv_all[pl.ds(me * blocks, blocks)] = kvsum.reshape(blocks, BLK, 2 * LANES)
    kv32[0] = kvsum[:, :LANES].astype(F32)
    kv32[1] = kvsum[:, LANES:].astype(F32)
    qsum = jnp.dot(tok[...], every[:, :qcols], preferred_element_type=F32)
    queries[...] = qsum.astype(BF).astype(F32)

    def kv_copy(d, slot):
        return pltpu.make_async_remote_copy(
            src_ref=kv_all.at[pl.ds(slot * blocks, blocks)],
            dst_ref=kv_all.at[pl.ds(slot * blocks, blocks)],
            send_sem=ks.at[d],
            recv_sem=kr.at[d],
            device_id={"kv": lax.rem(me + d, n)},
            device_id_type=MESH,
        )

    def comp_copy(d, slot):
        return pltpu.make_async_remote_copy(
            src_ref=comp_all.at[slot],
            dst_ref=comp_all.at[slot],
            send_sem=cs.at[d],
            recv_sem=cr.at[d],
            device_id={"kv": lax.rem(me + d, n)},
            device_id_type=MESH,
        )

    for d in range(1, n):

        @pl.when(me + d < n)
        def _():
            kv_copy(d, me).start()

    left = lax.broadcasted_iota(jnp.int32, (blocks, LANES), 1) < HEAD
    parts = []
    for which, weights in ((0, wck), (1, wcv)):
        source = kv32.at[which]
        flat[...] = jnp.zeros_like(flat)
        for pair in range(BLK // 2):
            even = source[pl.ds(2 * pair, blocks, stride=BLK), :]
            odd = source[pl.ds(2 * pair + 1, blocks, stride=BLK), :]
            span = pl.ds(pair * LANES, LANES)
            flat[0, 0:blocks, span] = jnp.where(left, even, pltpu.roll(odd, HEAD, 1))
            flat[1, 0:blocks, span] = jnp.where(left, pltpu.roll(even, HEAD, 1), odd)
        for g in range(groups):
            parts.append(
                lax.dot_general(flat[g].astype(BF), weights[...], dims, preferred_element_type=F32)
            )
    comp_all[me] = jnp.concatenate(parts, axis=1).astype(BF)
    for d in range(1, n):
        comp_copy(d, me).start()

    late = len(oring.items())
    early = 2 if share else late
    oring.relay(0, early)

    for d in range(1, n):

        @pl.when(me - d >= 0)
        def _():
            kv_copy(d, lax.rem(me - d + n, n)).wait_recv()

        comp_copy(d, lax.rem(me - d + n, n)).wait_recv()

    rows = per_group * BLK
    comp_pairs = comp_all[...].reshape(n * PAD, 2 * LANES)
    nkeys = (1 + depth) * BLK
    lane64 = lax.broadcasted_iota(jnp.int32, (BLK, LANES), 1) < HEAD
    comp_lane = lax.broadcasted_iota(jnp.int32, (rows, n * PAD), 1)
    comp_spot = lax.rem(lax.broadcasted_iota(jnp.int32, (rows, n * PAD), 0), BLK)
    comp_block = (comp_lane // PAD) * blocks + lax.rem(comp_lane, PAD)
    comp_real = lax.rem(comp_lane, PAD) < blocks
    key_lane = lax.broadcasted_iota(jnp.int32, (1, nkeys), 1)
    own_lane = lax.broadcasted_iota(jnp.int32, (rows, nkeys), 1)
    own_spot = lax.rem(lax.broadcasted_iota(jnp.int32, (rows, nkeys), 0), BLK)
    hidden = jnp.logical_and(own_lane < BLK, own_lane > own_spot)

    def pick_up(b, g):
        named = [slots[b, g, s] for s in range(depth)]

        def scan(c, held):
            block = kv_all[c]
            return tuple(lax.select(pick == c, block, old) for pick, old in zip(named, held))

        nothing = jnp.zeros((BLK, 2 * LANES), BF)
        found = lax.fori_loop(0, me * blocks, scan, (nothing,) * depth)
        for s in range(depth):
            near[g, (s + 1) * BLK : (s + 2) * BLK, :] = found[s]

    for g in range(groups if together else 0):
        pick_up(0, g)

    for b in range(blocks):
        spot = pl.ds(b * BLK, BLK)
        if b > 0 and early < late:
            oring.relay(early, early + 1)
            early += 1
        for g in range(groups):
            stacked = []
            for i in range(per_group):
                h = g * per_group + i
                tile = queries[spot, pl.ds((h // 2) * LANES, LANES)] * (HEAD**-0.5)
                if h % 2 != g:
                    tile = pltpu.roll(tile, HEAD, 1)
                keep = lane64 if g == 0 else jnp.logical_not(lane64)
                stacked.append(jnp.where(keep, tile, 0.0))
            qrows = jnp.concatenate(stacked, axis=0).astype(BF)

            comp_score = lax.dot_general(qrows, comp_pairs[:, :LANES], dims, preferred_element_type=F32)
            visible = jnp.logical_and(
                comp_real, (comp_block + 1) * BLK - 1 <= me * count + b * BLK + comp_spot
            )
            comp_score = jnp.where(visible, comp_score, masked_low)
            comp_top = jnp.max(comp_score, axis=1, keepdims=True)
            comp_weight = jnp.where(visible, jnp.exp(comp_score - comp_top), 0.0)
            comp_sum = jnp.maximum(jnp.sum(comp_weight, axis=1, keepdims=True), 1.0)
            comp_prob = (comp_weight * (1.0 / comp_sum)).astype(BF)
            comp_out = jnp.dot(comp_prob, comp_pairs[:, LANES:], preferred_element_type=F32)

            if not together:
                pick_up(b, g)
            near[g, 0:BLK, :] = kv_all[me * blocks + b]
            bias = jnp.zeros((1, nkeys), F32)
            for s in range(depth):
                bias = jnp.where(key_lane // BLK == s + 1, shuts[b, g, s], bias)
            score = lax.dot_general(qrows, near[g, :, :LANES], dims, preferred_element_type=F32) + bias
            score = jnp.where(hidden, masked_low, score)
            top = jnp.max(score, axis=1, keepdims=True)
            weight = jnp.exp(score - top)
            prob = (weight * (1.0 / jnp.sum(weight, axis=1, keepdims=True))).astype(BF)
            chosen_out = jnp.dot(prob, near[g, :, LANES:], preferred_element_type=F32)

            cols = [[], []]
            for i in range(per_group):
                for branch in (0, 1):
                    first = branch * all_heads + g * per_group + i
                    a = gates[spot, first : first + 1]
                    c = gates[spot, first + heads : first + heads + 1]
                    cols[branch].append(jnp.where(tp == 0, a, c))
            mixed = (
                jnp.concatenate(cols[0], axis=0) * comp_out
                + jnp.concatenate(cols[1], axis=0) * chosen_out
            )
            for j in range(per_group // 2):
                even = mixed[2 * j * BLK : (2 * j + 1) * BLK]
                odd = mixed[(2 * j + 1) * BLK : (2 * j + 2) * BLK]
                if g == 0:
                    odd = pltpu.roll(odd, HEAD, 1)
                else:
                    even = pltpu.roll(even, HEAD, 1)
                tile = g * (per_group // 2) + j
                att[spot, tile * LANES : (tile + 1) * LANES] = jnp.where(lane64, even, odd).astype(BF)

    oring.relay(early)
    oring.finish()

    def back(o):
        return pltpu.make_async_remote_copy(
            src_ref=sendbuf.at[o],
            dst_ref=recvbuf.at[o],
            send_sem=ts.at[o],
            recv_sem=tr.at[o],
            device_id={"tp": 1 - tp},
            device_id_type=MESH,
        )

    theirs = att[pl.ds(pl.multiple_of((1 - tp) * half, half), half), :]
    mine = att[pl.ds(pl.multiple_of(tp * half, half), half), :]
    for o in range(n):
        sendbuf[o] = jnp.dot(theirs, wout[o], preferred_element_type=F32).astype(BF)
        back(o).start()
    cols_each = wout.shape[2]
    live = (
        me * count + tp * half + lax.broadcasted_iota(jnp.int32, (half, cols_each), 0)
    ) < seq_ref[0]
    for o in range(n):
        kept = jnp.dot(mine, wout[o], preferred_element_type=F32).astype(BF).astype(F32)
        back(o).wait_recv()
        total = kept + recvbuf[o].astype(F32)
        out_ref[0, :, o * cols_each : (o + 1) * cols_each] = jnp.where(live, total, 0.0).astype(BF)

    ring.drain()
    oring.drain()
    for d in range(1, n):

        @pl.when(me + d < n)
        def _():
            kv_copy(d, me).wait_send()

        comp_copy(d, me).wait_send()
    for o in range(n):
        back(o).wait_send()


def solution(mesh):
    sizes = dict(mesh.shape)
    n = sizes["kv"]

    def body(tokens, seq_lengths, block_picks, wq, wk, wv, wg, wck, wcv, wo):
        _, count, width = tokens.shape
        blocks = count // BLK
        groups = wk.shape[1] // HEAD
        share = sizes["dp"] == 4 and (wq.shape[0] // 4) % 16 == 0 and n % 2 == 0
        steps = (2, n // 2, 2) if share else (1, n - 1, 1)
        depth = min(block_picks.shape[3], CAP * (n - 1))
        cols = wq.shape[1] + wk.shape[1] + wv.shape[1]
        half = count // sizes["tp"]
        sem = pltpu.SemaphoreType.DMA
        return pl.pallas_call(
            functools.partial(kernel, sizes, share),
            out_shape=jax.ShapeDtypeStruct((1, half, wo.shape[1] * n), BF),
            in_specs=[pl.BlockSpec(memory_space=pltpu.SMEM)] * 2
            + [pl.BlockSpec(memory_space=pl.ANY)] * 8,
            out_specs=pl.BlockSpec(memory_space=pltpu.VMEM),
            scratch_shapes=[
                pltpu.VMEM((count, width), BF),
                pltpu.VMEM((n, wq.shape[0], cols), BF),
                pltpu.VMEM((n,) + wo.shape, BF),
                pltpu.VMEM(wg.shape[::-1], BF),
                pltpu.VMEM(wck.shape[::-1], BF),
                pltpu.VMEM(wcv.shape[::-1], BF),
                pltpu.VMEM((count, wq.shape[1]), F32),
                pltpu.VMEM((2, count, LANES), F32),
                pltpu.VMEM((n * blocks, BLK, 2 * LANES), BF),
                pltpu.VMEM((groups, PAD, BLK * HEAD), F32),
                pltpu.VMEM((n, PAD, 2 * LANES), BF),
                pltpu.VMEM((count, wg.shape[1]), F32),
                pltpu.VMEM((count, wq.shape[1]), BF),
                pltpu.VMEM((groups, (1 + depth) * BLK, 2 * LANES), BF),
                pltpu.VMEM((n, half, wo.shape[1]), BF),
                pltpu.VMEM((n, half, wo.shape[1]), BF),
                pltpu.SMEM((blocks, groups, depth), jnp.int32),
                pltpu.SMEM((blocks, groups, depth), F32),
                sem((8,)),
            ]
            + [sem(steps)] * 8
            + [sem((n,))] * 6,
            compiler_params=pltpu.CompilerParams(
                collective_id=0, has_side_effects=True, vmem_limit_bytes=60 * 1024 * 1024
            ),
        )(seq_lengths, block_picks, tokens, wq, wk, wv, wg.T, wck.T, wcv.T, wo)

    return jax.shard_map(
        body,
        mesh=mesh,
        in_specs=(
            P("dp", "kv", None),
            P("dp"),
            P("dp", "kv", "tp", None),
            P("kv", "tp"),
            P("kv", "tp"),
            P("kv", "tp"),
            P(),
            P(),
            P(),
            P("tp", "kv"),
        ),
        out_specs=P("dp", ("kv", "tp"), None),
        check_vma=False,
    )
```
